32 devices in a mesh: ep: 8 (over z, core), tp: 4 (over y, x).
Axes of the slice: x: 2, y: 2, z: 4, core: 2. Of those that a mesh axis runs over, the one named last changes fastest.
Arguments:
- tokens: bfloat16 [4096, 2048], P(('ep', 'tp')), may hold values from -6 to 6
- norm_gain: float32 [2048], replicated, may hold values from 0.1 to 1.9
- expert_ids: int32 [4096, 2], P(('ep', 'tp')), may hold values from 0 to 7, all different within a row; in each aligned block of 128 rows (0 to 127, 128 to 255, ...) at most 64 rows name the same one
- gate_weights: float32 [4096, 2], P(('ep', 'tp')), may hold values from 0.2 to 1.6
- expert_gate: bfloat16 [8, 512, 2048], P('ep', 'tp'), may hold values from -0.125 to 0.125
- expert_up: bfloat16 [8, 512, 2048], P('ep', 'tp'), may hold values from -0.125 to 0.125
- expert_down: bfloat16 [8, 512, 2048], P('ep', 'tp'), may hold values from -0.25 to 0.25
- shared_gate: bfloat16 [512, 2048], P('tp'), may hold values from -0.125 to 0.125
- shared_up: bfloat16 [512, 2048], P('tp'), may hold values from -0.125 to 0.125
- shared_down: bfloat16 [512, 2048], P('tp'), may hold values from -0.25 to 0.25
Outputs:
- mixed: bfloat16 [4096, 2048], P(('ep', 'tp'))
The draws below stay inside these ranges and needn't reach their ends.
Inputs may be any that keep to these rules, and one draw needn't show every extreme that they name: `expert_ids`: each row names 2 different experts. Within the rows of one device no expert is named by more than 64 rows, and in every draw some expert is named by exactly 64 rows of some device.
All inputs are finite; a program needn't handle non-finite values.
Results may differ from the reference program's by a relative error of at most 0.0068.
Values may be sent and summed in bfloat16 or wider, within the bound.
No kernel may reach another device: no remote copies, remote signals or barrier semaphores. Data moves between devices by JAX's collectives and lax.ppermute only.
A program may use at most 64 MiB of HBM per device.

```python
import math
import jax
import jax.numpy as jnp
import numpy as np
from jax import lax

D = 2048
FF = 512
SFF = 512
K = 2
TOK_DEV = 128
EXPERTS = 8
CAP = 64
TOKENS = 4096


def block_levels(rng, shape, shards, smallest, largest):
    gain = 1.0
    for dim, parts in shards:
        draws = jax.random.uniform(jax.random.fold_in(jax.random.fold_in(rng, 6), dim), (parts,), jnp.float32, smallest / len(shards), largest / len(shards))
        gain = gain * jnp.repeat(jnp.exp(draws), shape[dim] // parts).reshape((-1,) + (1,) * (len(shape) - 1 - dim))
    return gain


def deal_out(own_key, own, number, rows, amount, top, limit, skew):
    sequence = jax.random.permutation(own_key, amount)
    packed, common = shares(amount, rows * top, limit, skew, True), shares(amount, rows * top, limit, skew, False)
    places = jnp.arange(amount)

    def named(tallies, turn):
        used = int((tallies > 0).sum())
        fixed = max(1, used // 4)
        shifted = fixed + (places - fixed + turn * (used - fixed)) % max(1, amount - fixed)
        return jnp.zeros((amount,), jnp.int32).at[sequence[jnp.where(places < fixed, places, shifted)]].set(jnp.asarray(tallies, jnp.int32))

    tallies = jnp.where(number % 4 == 0, named(packed, number // 4), named(common, number - number // 4 - 1))
    mixed = jax.random.permutation(jax.random.fold_in(own, 3), amount)
    giver, taker = mixed[0:amount // 2 * 2:2], mixed[1:amount // 2 * 2:2]
    slack = jnp.minimum(tallies[giver] - 1, limit - tallies[taker]) // 2
    slack = jnp.where((giver == sequence[0]) | (taker == sequence[0]) | (tallies[taker] == 0), 0, jnp.maximum(slack, 0))
    shifted = jax.random.randint(jax.random.fold_in(own, 4), (amount // 2,), 0, 1 << 20) % (slack + 1)
    tallies = tallies.at[giver].add(-shifted).at[taker].add(shifted)
    members = jnp.searchsorted(jnp.cumsum(tallies), jnp.arange(rows * top), side="right").astype(jnp.int32)
    listing = members.reshape(top, rows).T
    listing = listing[jax.random.permutation(jax.random.fold_in(own, 1), rows)]
    turn = jax.random.randint(jax.random.fold_in(own, 2), (rows, 1), 0, top)
    return jnp.take_along_axis(listing, (jnp.arange(top)[None, :] + turn) % top, axis=1)


def shares(amount, total, bound, lean, full):
    portions = [(1 << 20) // math.isqrt(standing ** lean) + 1 for standing in range(1, amount + 1)]
    largest = bound if full else min(bound, max(-(-total // amount), total * portions[0] // sum(portions)))
    least = 1 if total - largest >= amount - 1 else 0
    counts, rest = [largest] + [least] * (amount - 1), total - largest - least * (amount - 1)
    while rest > 0:
        free = [i for i in range(1, amount) if counts[i] < largest] or [i for i in range(1, amount) if counts[i] < bound]
        mass, left = sum([portions[i] for i in free]), rest
        for i in free:
            addition = min(bound - counts[i], max(1, left * portions[i] // mass), rest)
            counts[i] = counts[i] + addition
            rest = rest - addition
    return np.array(counts)


def normal_values(rng, extent, spread, reach, pieces=(), held_as=jnp.bfloat16):
    values = spread * jax.random.normal(rng, extent, jnp.float32)
    if pieces:
        values = values * block_levels(rng, extent, pieces, -0.22, 0.18)
    return jnp.clip(values, -reach, reach).astype(held_as)


def setup_inputs(seed: int = 0) -> dict:
    seeds = jax.random.split(jax.random.key(seed), 11)
    tokens = normal_values(seeds[0], (TOKENS, D), 1.0, 6.0, ((0, 32),))
    norm_gain = jnp.clip(1.0 + 0.18 * jax.random.normal(seeds[1], (D,), jnp.float32), 0.1, 1.9)
    expert_ids_keys = jax.random.split(jax.random.fold_in(seeds[2], 1), TOKENS // TOK_DEV)
    expert_ids_turns = jax.random.permutation(jax.random.fold_in(seeds[2], 3), TOKENS // TOK_DEV)
    expert_ids = jax.vmap(lambda own, number: deal_out(jax.random.fold_in(seeds[2], 2), own, number, TOK_DEV, EXPERTS, K, CAP, 2))(expert_ids_keys, expert_ids_turns).reshape((TOKENS, K))
    gate_weights = jnp.clip(0.2 + 1.4 * jax.random.uniform(seeds[3], (TOKENS, K), jnp.float32) ** block_levels(seeds[3], (TOKENS, K), ((0, 32),), -0.2, 0.2), 0.2, 1.6)
    expert_gate = normal_values(seeds[4], (EXPERTS, FF, D), D ** -0.5, 0.125, ((0, 8), (1, 4)))
    expert_up = normal_values(seeds[5], (EXPERTS, FF, D), D ** -0.5, 0.125, ((0, 8), (1, 4)))
    expert_down = normal_values(seeds[6], (EXPERTS, FF, D), FF ** -0.5, 0.25, ((0, 8), (1, 4)))
    shared_gate = normal_values(seeds[7], (SFF, D), D ** -0.5, 0.125, ((0, 4),))
    shared_up = normal_values(seeds[8], (SFF, D), D ** -0.5, 0.125, ((0, 4),))
    shared_down = normal_values(seeds[9], (SFF, D), SFF ** -0.5, 0.25, ((0, 4),))
    return {"tokens": tokens, "norm_gain": norm_gain, "expert_ids": expert_ids, "gate_weights": gate_weights, "expert_gate": expert_gate, "expert_up": expert_up, "expert_down": expert_down, "shared_gate": shared_gate, "shared_up": shared_up, "shared_down": shared_down}


EPS = 1e-06

def against(rows, weight):
    return jnp.dot(rows, weight.T, preferred_element_type=jnp.float32)

def reference(tokens, norm_gain, expert_ids, gate_weights, expert_gate, expert_up, expert_down, shared_gate, shared_up, shared_down):
    tok = tokens.astype(jnp.float32)
    normed = (tok * lax.rsqrt(lax.optimization_barrier(jnp.mean(tok * tok, axis=-1, keepdims=True)) + EPS) * norm_gain).astype(jnp.bfloat16)
    most_rows = TOKENS // TOK_DEV * CAP
    order = jnp.arange(TOKENS, dtype=jnp.int32)

    def one_expert(index, routed):
        named = expert_ids == index
        member = jnp.any(named, axis=1).astype(jnp.int32)
        weight_row = lax.optimization_barrier(jnp.sum(jnp.where(named, gate_weights, 0.0), axis=1))
        place = (jnp.cumsum(member) - member).astype(jnp.int32)
        place = jnp.where(member > 0, place, most_rows).astype(jnp.int32)
        table = jnp.full((most_rows,), TOKENS, jnp.int32).at[place].set(order, mode='drop')
        rows = jnp.take(normed, table, axis=0, mode='fill', fill_value=0)
        scale = jnp.take(weight_row, table, axis=0, mode='fill', fill_value=0)
        gate = lax.dynamic_index_in_dim(expert_gate, index, 0, keepdims=False)
        up = lax.dynamic_index_in_dim(expert_up, index, 0, keepdims=False)
        down = lax.dynamic_index_in_dim(expert_down, index, 0, keepdims=False)
        hidden = (jax.nn.silu(against(rows, gate)) * against(rows, up)).astype(jnp.bfloat16)
        result = jnp.dot(hidden, down, preferred_element_type=jnp.float32).astype(jnp.bfloat16)
        return routed.at[table].add(scale[:, None] * result.astype(jnp.float32), mode='drop')
    routed = lax.fori_loop(0, EXPERTS, one_expert, jnp.zeros((TOKENS, D), jnp.float32))
    shared_hidden = (jax.nn.silu(against(normed, shared_gate)) * against(normed, shared_up)).astype(jnp.bfloat16)
    shared = jnp.dot(shared_hidden, shared_down, preferred_element_type=jnp.float32)
    return (routed + shared).astype(jnp.bfloat16)
```

```python
import jax
import jax.numpy as jnp
from jax import lax
from jax.sharding import PartitionSpec as P

EPS = 1e-06


def for_sending(shard):
    return jax.tree.map(lambda a: a.astype(jnp.bfloat16) if a.dtype == jnp.float32 else a, shard)


def against(rows, weight):
    return lax.dot_general(
        rows, weight, (((1,), (1,)), ((), ())), preferred_element_type=jnp.float32
    )


def hidden_block(rows, gate_rows, up_rows):
    return (jax.nn.silu(against(rows, gate_rows)) * against(rows, up_rows)).astype(jnp.bfloat16)


def apart_mlp(rows, gate, up, down, width, collect_pair, collect_rest):

    def fill_hidden(hidden, pieces, start):
        block = hidden_block(rows, pieces[0], pieces[1])
        return block

    hidden = collect_pair((gate, up), fill_hidden, jnp.zeros((rows.shape[0], width), jnp.bfloat16))

    def add_down(total, piece, start):
        return jnp.dot(hidden, piece, preferred_element_type=jnp.float32)

    empty = jnp.zeros((rows.shape[0], down.shape[1]), jnp.float32)
    return collect_rest(down, add_down, empty)


def exchange_body(
    tokens,
    norm_gain,
    expert_ids,
    gate_weights,
    expert_gate,
    expert_up,
    expert_down,
    shared_gate,
    shared_up,
    shared_down,
):
    tok = tokens.astype(jnp.float32)
    normed = (
        tok * lax.rsqrt(jnp.mean(tok * tok, axis=-1, keepdims=True) + EPS) * norm_gain
    ).astype(jnp.bfloat16)
    groups = lax.axis_size("tp")
    count = lax.axis_size("ep")
    tok_rows, chosen = expert_ids.shape
    features = tokens.shape[1]
    capacity = 2 * tok_rows * chosen // count
    labels = jnp.arange(count, dtype=jnp.int32)
    hits = jnp.sum((expert_ids[:, :, None] == labels[None, None, :]).astype(jnp.int32), axis=1)
    before = jnp.cumsum(hits, axis=0) - hits
    slot_of = jnp.take_along_axis(before, expert_ids, axis=1)
    flat_pos = expert_ids * capacity + slot_of
    slots = jnp.arange(count * capacity, dtype=jnp.int32)
    placing = jnp.any(flat_pos[:, :, None] == slots[None, None, :], axis=1).astype(jnp.bfloat16)
    outgoing = lax.dot_general(
        placing, normed, (((0,), (0,)), ((), ())), preferred_element_type=jnp.float32
    )
    outgoing = outgoing.astype(jnp.bfloat16).reshape(count, capacity, features)
    arrived = lax.all_to_all(outgoing, "ep", split_axis=0, concat_axis=0, tiled=True)
    rows = arrived.reshape(count * capacity, features)
    width = expert_gate.shape[1] * groups
    results = apart_mlp(
        rows,
        expert_gate[0],
        expert_up[0],
        expert_down[0],
        width,
        lambda x, fn, init: fn(
            init,
            jax.tree.map(lambda a: lax.all_gather(a, "tp", axis=0, tiled=True), for_sending(x)),
            jnp.int32(0),
        ),
        lambda x, fn, init: fn(init, lax.all_gather(x, "tp", axis=0, tiled=True), jnp.int32(0)),
    )
    results = results.astype(jnp.bfloat16).reshape(count, capacity, features)
    returned = lax.all_to_all(results, "ep", split_axis=0, concat_axis=0, tiled=True).reshape(
        count * capacity, features
    )
    picked = jnp.take(returned, flat_pos.reshape(-1), axis=0).reshape(tok_rows, chosen, features)
    routed = jnp.sum(gate_weights[:, :, None] * picked.astype(jnp.float32), axis=1)
    width = shared_gate.shape[0] * groups
    shared = apart_mlp(
        normed,
        shared_gate,
        shared_up,
        shared_down,
        width,
        lambda x, fn, init: fn(
            init,
            jax.tree.map(lambda a: lax.all_gather(a, "tp", axis=0, tiled=True), for_sending(x)),
            jnp.int32(0),
        ),
        lambda x, fn, init: fn(init, lax.all_gather(x, "tp", axis=0, tiled=True), jnp.int32(0)),
    )
    return (routed + shared).astype(jnp.bfloat16)


CORES = 2
CHUNKS = 4


def column_body(
    tokens,
    norm_gain,
    expert_ids,
    gate_weights,
    expert_gate,
    expert_up,
    expert_down,
    shared_gate,
    shared_up,
    shared_down,
):
    ep, tp = lax.axis_size("ep"), lax.axis_size("tp")
    levels = ep // CORES
    me = lax.axis_index("ep")
    tok_rows, features = tokens.shape

    z_up = [(i, (i + CORES) % ep) for i in range(ep)]
    swap = [(i, i ^ 1) for i in range(ep)]
    x_swap = [(i, i ^ 1) for i in range(tp)]
    y_swap = [(i, i ^ 2) for i in range(tp)]

    def up(a):
        return lax.ppermute(a, "ep", z_up)

    def other_core(a):
        return lax.ppermute(a, "ep", swap)

    def over_x(a):
        return lax.ppermute(a, "tp", x_swap)

    def over_y(a):
        return lax.ppermute(a, "tp", y_swap)

    own_shared = shared_gate.shape[0] // ep

    def with_shared(routed, shared):
        mine = lax.dynamic_slice_in_dim(shared, me * own_shared, own_shared, 0)
        return jnp.concatenate([routed[0], mine], axis=0)

    gate = with_shared(expert_gate, shared_gate)
    upw = with_shared(expert_up, shared_up)
    down = with_shared(expert_down, shared_down)
    units = gate.shape[0]
    half = units // 2
    is_routed = jnp.arange(units) < expert_gate.shape[1]

    labels = jnp.arange(ep, dtype=jnp.int32)
    dense = jnp.sum(
        jnp.where(expert_ids[:, :, None] == labels, gate_weights[:, :, None], 0.0), axis=1
    )
    high = dense.astype(jnp.bfloat16)
    low = (dense - high.astype(jnp.float32)).astype(jnp.bfloat16)
    pad = jnp.zeros((tok_rows, 128 - 2 * ep), jnp.bfloat16)
    block = jnp.concatenate([tokens, high, low, pad], axis=1)

    ga, gb = (jnp.concatenate([gate[s], upw[s]], axis=0) for s in (slice(0, half), slice(half, None)))
    xa = over_x(ga)
    yb = over_y(gb)
    ya = over_y(ga)
    xb = over_x(gb)
    da = over_y(xa)
    db = over_x(yb)

    own_blocks, other_blocks = [block], [other_core(block)]
    for _ in range(levels - 1):
        own_blocks.append(up(own_blocks[-1]))
        other_blocks.append(other_core(own_blocks[-1]))
    order = list(range(1, levels)) + [0]
    column = jnp.concatenate([own_blocks[r] for r in order] + [other_blocks[r] for r in order], axis=0)

    tok = column[:, :features].astype(jnp.float32)
    normed = (
        tok * lax.rsqrt(jnp.mean(tok * tok, axis=-1, keepdims=True) + EPS) * norm_gain
    ).astype(jnp.bfloat16)
    coded = column[:, features : features + 2 * ep].astype(jnp.float32)
    coded = coded[:, :ep] + coded[:, ep:]
    weight = jnp.sum(jnp.where(labels == me, coded, 0.0), axis=1, keepdims=True)

    def hidden_of(pieces, routed):
        g = jnp.concatenate([p[: p.shape[0] // 2] for p in pieces], axis=0)
        u = jnp.concatenate([p[p.shape[0] // 2 :] for p in pieces], axis=0)
        value = jax.nn.silu(against(normed, g)) * against(normed, u)
        return (value * jnp.where(routed[None, :], weight, 1.0)).astype(jnp.bfloat16)

    near = hidden_of([ga, gb, xa, xb, ya, yb], jnp.concatenate([is_routed] * 3))
    far = hidden_of([da, db], is_routed)
    hidden = jnp.concatenate([near, far], axis=1)

    own_rows = levels * tok_rows
    width = features // CHUNKS
    outs = []
    for c in range(CHUNKS):
        piece = down[:, c * width : (c + 1) * width]
        dx, dy = over_x(piece), over_y(piece)
        dda, ddb = over_y(dx[:half]), over_x(dy[half:])
        rows = jnp.concatenate([piece, dx, dy, dda, ddb], axis=0)
        part = jnp.dot(hidden, rows, preferred_element_type=jnp.float32)
        total = part[:own_rows] + other_core(part[own_rows:].astype(jnp.bfloat16)).astype(jnp.float32)
        moving = total[:tok_rows]
        for r in range(1, levels):
            arrived = up(moving.astype(jnp.bfloat16)).astype(jnp.float32)
            moving = total[r * tok_rows : (r + 1) * tok_rows] + arrived
        outs.append(moving.astype(jnp.bfloat16))
    return jnp.concatenate(outs, axis=1)


def solution(mesh):
    ep, tp = mesh.shape["ep"], mesh.shape["tp"]
    body = column_body if tp == 4 and ep % CORES == 0 and ep <= 8 else exchange_body
    in_specs = (
        P(("ep", "tp"), None),
        P(),
        P(("ep", "tp"), None),
        P(("ep", "tp"), None),
        P("ep", "tp", None),
        P("ep", "tp", None),
        P("ep", "tp", None),
        P("tp", None),
        P("tp", None),
        P("tp", None),
    )
    out_specs = P(("ep", "tp"), None)
    return jax.shard_map(body, mesh=mesh, in_specs=in_specs, out_specs=out_specs, check_vma=False)
```

```python
import jax
import jax.numpy as jnp
from jax import lax
from jax.experimental import pallas as pl
from jax.experimental.pallas import tpu as pltpu
from jax.experimental.layout import Layout, with_layout_constraint
from jax.sharding import PartitionSpec as P

EPS = 1e-06


def for_sending(shard):
    return jax.tree.map(lambda a: a.astype(jnp.bfloat16) if a.dtype == jnp.float32 else a, shard)


def against(rows, weight):
    return lax.dot_general(
        rows, weight, (((1,), (1,)), ((), ())), preferred_element_type=jnp.float32
    )


def hidden_block(rows, gate_rows, up_rows):
    return (jax.nn.silu(against(rows, gate_rows)) * against(rows, up_rows)).astype(jnp.bfloat16)


def apart_mlp(rows, gate, up, down, width, collect_pair, collect_rest):

    def fill_hidden(hidden, pieces, start):
        block = hidden_block(rows, pieces[0], pieces[1])
        return block

    hidden = collect_pair((gate, up), fill_hidden, jnp.zeros((rows.shape[0], width), jnp.bfloat16))

    def add_down(total, piece, start):
        return jnp.dot(hidden, piece, preferred_element_type=jnp.float32)

    empty = jnp.zeros((rows.shape[0], down.shape[1]), jnp.float32)
    return collect_rest(down, add_down, empty)


def exchange_body(
    tokens,
    norm_gain,
    expert_ids,
    gate_weights,
    expert_gate,
    expert_up,
    expert_down,
    shared_gate,
    shared_up,
    shared_down,
):
    tok = tokens.astype(jnp.float32)
    normed = (
        tok * lax.rsqrt(jnp.mean(tok * tok, axis=-1, keepdims=True) + EPS) * norm_gain
    ).astype(jnp.bfloat16)
    groups = lax.axis_size("tp")
    count = lax.axis_size("ep")
    tok_rows, chosen = expert_ids.shape
    features = tokens.shape[1]
    capacity = 2 * tok_rows * chosen // count
    labels = jnp.arange(count, dtype=jnp.int32)
    hits = jnp.sum((expert_ids[:, :, None] == labels[None, None, :]).astype(jnp.int32), axis=1)
    before = jnp.cumsum(hits, axis=0) - hits
    slot_of = jnp.take_along_axis(before, expert_ids, axis=1)
    flat_pos = expert_ids * capacity + slot_of
    slots = jnp.arange(count * capacity, dtype=jnp.int32)
    placing = jnp.any(flat_pos[:, :, None] == slots[None, None, :], axis=1).astype(jnp.bfloat16)
    outgoing = lax.dot_general(
        placing, normed, (((0,), (0,)), ((), ())), preferred_element_type=jnp.float32
    )
    outgoing = outgoing.astype(jnp.bfloat16).reshape(count, capacity, features)
    arrived = lax.all_to_all(outgoing, "ep", split_axis=0, concat_axis=0, tiled=True)
    rows = arrived.reshape(count * capacity, features)
    width = expert_gate.shape[1] * groups
    results = apart_mlp(
        rows,
        expert_gate[0],
        expert_up[0],
        expert_down[0],
        width,
        lambda x, fn, init: fn(
            init,
            jax.tree.map(lambda a: lax.all_gather(a, "tp", axis=0, tiled=True), for_sending(x)),
            jnp.int32(0),
        ),
        lambda x, fn, init: fn(init, lax.all_gather(x, "tp", axis=0, tiled=True), jnp.int32(0)),
    )
    results = results.astype(jnp.bfloat16).reshape(count, capacity, features)
    returned = lax.all_to_all(results, "ep", split_axis=0, concat_axis=0, tiled=True).reshape(
        count * capacity, features
    )
    picked = jnp.take(returned, flat_pos.reshape(-1), axis=0).reshape(tok_rows, chosen, features)
    routed = jnp.sum(gate_weights[:, :, None] * picked.astype(jnp.float32), axis=1)
    width = shared_gate.shape[0] * groups
    shared = apart_mlp(
        normed,
        shared_gate,
        shared_up,
        shared_down,
        width,
        lambda x, fn, init: fn(
            init,
            jax.tree.map(lambda a: lax.all_gather(a, "tp", axis=0, tiled=True), for_sending(x)),
            jnp.int32(0),
        ),
        lambda x, fn, init: fn(init, lax.all_gather(x, "tp", axis=0, tiled=True), jnp.int32(0)),
    )
    return (routed + shared).astype(jnp.bfloat16)


CORES = 2
CHUNKS = 4


def copy_blocks(jobs, arrays, shapes, at=None):
    def kernel(at_ref, *refs):
        ins, outs, sem = refs[: len(arrays)], refs[len(arrays) : -1], refs[-1]
        copies = []
        for n, (source, row, rows, cols, target, to) in enumerate(jobs):
            if row is None:
                row = pl.multiple_of(at_ref[0], rows)
            copies.append(
                pltpu.make_async_copy(
                    ins[source].at[pl.ds(row, rows), cols],
                    outs[target].at[pl.ds(to, rows)],
                    sem.at[n],
                )
            )
        for copy in copies:
            copy.start()
        for copy in copies:
            copy.wait()

    at = jnp.zeros((1,), jnp.int32) if at is None else at
    moved = sum(s[0] * s[1] for s in shapes) * 2
    return pl.pallas_call(
        kernel,
        out_shape=[jax.ShapeDtypeStruct(s, jnp.bfloat16) for s in shapes],
        in_specs=[pl.BlockSpec(memory_space=pltpu.SMEM)]
        + [pl.BlockSpec(memory_space=pltpu.HBM)] * len(arrays),
        out_specs=[pl.BlockSpec(memory_space=pltpu.VMEM)] * len(shapes),
        scratch_shapes=[pltpu.SemaphoreType.DMA((len(jobs),))],
        compiler_params=pltpu.CompilerParams(vmem_limit_bytes=8 * 1024 * 1024),
        cost_estimate=pl.CostEstimate(flops=moved, bytes_accessed=2 * moved, transcendentals=0),
    )(at, *arrays)


def column_body(
    tokens,
    norm_gain,
    expert_ids,
    gate_weights,
    expert_gate,
    expert_up,
    expert_down,
    shared_gate,
    shared_up,
    shared_down,
):
    ep, tp = lax.axis_size("ep"), lax.axis_size("tp")
    levels = ep // CORES
    me = lax.axis_index("ep")
    tok_rows, features = tokens.shape

    z_up = [(i, (i + CORES) % ep) for i in range(ep)]
    swap = [(i, i ^ 1) for i in range(ep)]
    x_swap = [(i, i ^ 1) for i in range(tp)]
    y_swap = [(i, i ^ 2) for i in range(tp)]
    both_swap = [(i, i ^ 3) for i in range(tp)]

    def over_x(a):
        return lax.ppermute(a, "tp", x_swap)

    def over_y(a):
        return lax.ppermute(a, "tp", y_swap)

    def across(a):
        return lax.ppermute(a, "tp", both_swap)

    def up(a):
        return lax.ppermute(a, "ep", z_up)

    def other_core(a):
        return lax.ppermute(a, "ep", swap)

    s = shared_gate.shape[0] // ep
    features = tokens.shape[1]
    every = slice(0, features)
    shared = copy_blocks(
        [(i, None, s, every, 0, i * s) for i in range(3)],
        (shared_gate, shared_up, shared_down),
        [(3 * s, features)],
        at=(me * s).astype(jnp.int32)[None],
    )[0]
    gate, upw, down = expert_gate[0], expert_up[0], expert_down[0]

    labels = jnp.arange(ep, dtype=jnp.int32)[:, None]
    dense = sum(
        jnp.where(expert_ids[None, :, k] == labels, gate_weights[None, :, k], 0.0)
        for k in range(expert_ids.shape[1])
    )

    gx, gy = over_x(gate), over_y(gate)
    ux, uy = over_x(upw), over_y(upw)
    sx, sy, sd = over_x(shared), over_y(shared), across(shared)
    gd, ud = over_y(gx), over_x(uy)

    own_blocks, other_blocks = [tokens], [other_core(tokens)]
    weights = [jnp.concatenate([dense, other_core(dense)], axis=0)]
    for _ in range(1, levels):
        own_blocks.append(up(own_blocks[-1]))
        other_blocks.append(other_core(own_blocks[-1]))
        weights.append(up(weights[-1]))

    quarter = features // CHUNKS
    down_rows = []
    for n, (lo, hi) in enumerate(((0, 1), (1, 2), (2, 4))):
        piece = down[:, lo * quarter : hi * quarter]
        dx, dy = over_x(piece), over_y(piece)
        dd = across(piece)
        down_rows.append((piece, dx, dy, dd))

    def normed_of(part):
        tok = part.astype(jnp.float32)
        factor = lax.rsqrt(jnp.mean(tok * tok, axis=-1, keepdims=True) + EPS)
        return (tok * factor * norm_gain).astype(jnp.bfloat16)

    def joined(pieces):
        return jnp.concatenate(pieces, axis=0)

    order = list(range(1, levels)) + [0]
    shares = (shared, sx, sy, sd)
    n = gate.shape[0]
    units = 4 * n + 4 * s
    places = (0, n, 2 * n, 3 * n)
    arrays = (gate, gx, gy, gd, upw, ux, uy, ud, *shares)
    jobs = [(i, 0, n, every, i // 4, places[i % 4]) for i in range(8)]
    jobs += [(8 + i, t * s, s, every, t, 4 * n + i * s) for i in range(4) for t in range(2)]
    g_all, u_all = copy_blocks(jobs, arrays, [(units, features)] * 2)
    weights = lax.optimization_barrier((*weights, g_all))[:-1]

    rows = joined(
        [normed_of(own_blocks[r]) for r in order] + [normed_of(other_blocks[r]) for r in order]
    )
    picked = [lax.dynamic_slice_in_dim(weights[r].reshape(2, ep, -1), me, 1, 1) for r in order]
    scale = joined([p[c, 0] for c in range(2) for p in picked])[:, None]
    routed = (jnp.arange(units) < 4 * n)[None, :]
    value = jax.nn.silu(against(rows, g_all)) * against(rows, u_all)
    hidden = (value * jnp.where(routed, scale, 1.0)).astype(jnp.bfloat16)

    own_rows = levels * tok_rows

    def product(c, lo, hi):
        arrays = (*down_rows[c], *shares)
        jobs = [(i, 0, n, slice(0, hi - lo), 0, i * n) for i in range(4)]
        jobs += [(4 + i, 2 * s, s, slice(lo, hi), 0, 4 * n + i * s) for i in range(4)]
        down_all = copy_blocks(jobs, arrays, [(units, hi - lo)])[0]
        part = jnp.dot(hidden, down_all, preferred_element_type=jnp.float32)
        return with_layout_constraint(part, Layout(major_to_minor=(0, 1)))

    parts = [product(0, 0, quarter), product(1, quarter, 2 * quarter)]
    wide = product(2, 2 * quarter, features)
    parts += [wide[:, :quarter], wide[:, quarter:]]
    outs = []
    for part in parts:
        swapped = other_core(part[own_rows:].astype(jnp.bfloat16))
        total = part[:own_rows] + swapped.astype(jnp.float32)
        moving = total[:tok_rows]
        for r in range(1, levels):
            arrived = up(moving.astype(jnp.bfloat16))
            moving = total[r * tok_rows : (r + 1) * tok_rows] + arrived.astype(jnp.float32)
        outs.append(moving.astype(jnp.bfloat16))
    return jnp.concatenate(outs, axis=1)


def solution(mesh):
    ep, tp = mesh.shape["ep"], mesh.shape["tp"]
    columns = tp == 4 and ep == 4 * CORES

    def body(*args):
        return (column_body if columns else exchange_body)(*args)

    in_specs = (
        P(("ep", "tp"), None),
        P(),
        P(("ep", "tp"), None),
        P(("ep", "tp"), None),
        P("ep", "tp", None),
        P("ep", "tp", None),
        P("ep", "tp", None),
        P("tp", None),
        P("tp", None),
        P("tp", None),
    )
    out_specs = P(("ep", "tp"), None)
    return jax.shard_map(
        body, mesh=mesh, in_specs=in_specs, out_specs=out_specs, check_vma=False
    )
```

```python
import jax
import jax.numpy as jnp
from functools import partial

from jax import lax
from jax.experimental import pallas as pl
from jax.experimental.pallas import tpu as pltpu
from jax.experimental.layout import Layout, with_layout_constraint
from jax.sharding import PartitionSpec as P

EPS = 1e-06


def for_sending(shard):
    return jax.tree.map(lambda a: a.astype(jnp.bfloat16) if a.dtype == jnp.float32 else a, shard)


def against(rows, weight):
    return lax.dot_general(
        rows, weight, (((1,), (1,)), ((), ())), preferred_element_type=jnp.float32
    )


def hidden_block(rows, gate_rows, up_rows):
    return (jax.nn.silu(against(rows, gate_rows)) * against(rows, up_rows)).astype(jnp.bfloat16)


def apart_mlp(rows, gate, up, down, width, collect_pair, collect_rest):

    def fill_hidden(hidden, pieces, start):
        block = hidden_block(rows, pieces[0], pieces[1])
        return block

    hidden = collect_pair((gate, up), fill_hidden, jnp.zeros((rows.shape[0], width), jnp.bfloat16))

    def add_down(total, piece, start):
        return jnp.dot(hidden, piece, preferred_element_type=jnp.float32)

    empty = jnp.zeros((rows.shape[0], down.shape[1]), jnp.float32)
    return collect_rest(down, add_down, empty)


def exchange_body(
    tokens,
    norm_gain,
    expert_ids,
    gate_weights,
    expert_gate,
    expert_up,
    expert_down,
    shared_gate,
    shared_up,
    shared_down,
):
    tok = tokens.astype(jnp.float32)
    normed = (
        tok * lax.rsqrt(jnp.mean(tok * tok, axis=-1, keepdims=True) + EPS) * norm_gain
    ).astype(jnp.bfloat16)
    groups = lax.axis_size("tp")
    count = lax.axis_size("ep")
    tok_rows, chosen = expert_ids.shape
    features = tokens.shape[1]
    capacity = 2 * tok_rows * chosen // count
    labels = jnp.arange(count, dtype=jnp.int32)
    hits = jnp.sum((expert_ids[:, :, None] == labels[None, None, :]).astype(jnp.int32), axis=1)
    before = jnp.cumsum(hits, axis=0) - hits
    slot_of = jnp.take_along_axis(before, expert_ids, axis=1)
    flat_pos = expert_ids * capacity + slot_of
    slots = jnp.arange(count * capacity, dtype=jnp.int32)
    placing = jnp.any(flat_pos[:, :, None] == slots[None, None, :], axis=1).astype(jnp.bfloat16)
    outgoing = lax.dot_general(
        placing, normed, (((0,), (0,)), ((), ())), preferred_element_type=jnp.float32
    )
    outgoing = outgoing.astype(jnp.bfloat16).reshape(count, capacity, features)
    arrived = lax.all_to_all(outgoing, "ep", split_axis=0, concat_axis=0, tiled=True)
    rows = arrived.reshape(count * capacity, features)
    width = expert_gate.shape[1] * groups
    results = apart_mlp(
        rows,
        expert_gate[0],
        expert_up[0],
        expert_down[0],
        width,
        lambda x, fn, init: fn(
            init,
            jax.tree.map(lambda a: lax.all_gather(a, "tp", axis=0, tiled=True), for_sending(x)),
            jnp.int32(0),
        ),
        lambda x, fn, init: fn(init, lax.all_gather(x, "tp", axis=0, tiled=True), jnp.int32(0)),
    )
    results = results.astype(jnp.bfloat16).reshape(count, capacity, features)
    returned = lax.all_to_all(results, "ep", split_axis=0, concat_axis=0, tiled=True).reshape(
        count * capacity, features
    )
    picked = jnp.take(returned, flat_pos.reshape(-1), axis=0).reshape(tok_rows, chosen, features)
    routed = jnp.sum(gate_weights[:, :, None] * picked.astype(jnp.float32), axis=1)
    width = shared_gate.shape[0] * groups
    shared = apart_mlp(
        normed,
        shared_gate,
        shared_up,
        shared_down,
        width,
        lambda x, fn, init: fn(
            init,
            jax.tree.map(lambda a: lax.all_gather(a, "tp", axis=0, tiled=True), for_sending(x)),
            jnp.int32(0),
        ),
        lambda x, fn, init: fn(init, lax.all_gather(x, "tp", axis=0, tiled=True), jnp.int32(0)),
    )
    return (routed + shared).astype(jnp.bfloat16)


CORES = 2
CHUNKS = 4


def copy_blocks(jobs, arrays, shapes, me):
    def kernel(me_ref, *refs):
        ins, outs, sem = refs[: len(arrays)], refs[len(arrays) : -1], refs[-1]
        copies = []
        for n, (source, row, rows, cols, target, to) in enumerate(jobs):
            row, to = (
                pl.multiple_of(place(me_ref[0]), rows) if callable(place) else place
                for place in (row, to)
            )
            copies.append(
                pltpu.make_async_copy(
                    ins[source].at[pl.ds(row, rows), cols],
                    outs[target].at[pl.ds(to, rows)],
                    sem.at[n],
                )
            )
        for copy in copies:
            copy.start()
        for copy in copies:
            copy.wait()

    moved = sum(s[0] * s[1] for s in shapes) * 2
    return pl.pallas_call(
        kernel,
        out_shape=[jax.ShapeDtypeStruct(s, jnp.bfloat16) for s in shapes],
        in_specs=[pl.BlockSpec(memory_space=pltpu.SMEM)]
        + [pl.BlockSpec(memory_space=pltpu.HBM)] * len(arrays),
        out_specs=[pl.BlockSpec(memory_space=pltpu.VMEM)] * len(shapes),
        scratch_shapes=[pltpu.SemaphoreType.DMA((len(jobs),))],
        compiler_params=pltpu.CompilerParams(vmem_limit_bytes=24 * 1024 * 1024),
        cost_estimate=pl.CostEstimate(flops=moved, bytes_accessed=2 * moved, transcendentals=0),
    )(me, *arrays)


def norm_kernel(tok_ref, gain_ref, out_ref):
    def step(i, carry):
        tile = pl.ds(pl.multiple_of(i * 16, 16), 16)
        tok = tok_ref[tile].astype(jnp.float32)
        factor = lax.rsqrt(jnp.mean(tok * tok, axis=-1, keepdims=True) + EPS)
        out_ref[tile] = (tok * factor * gain_ref[...]).astype(jnp.bfloat16)
        return carry

    lax.fori_loop(0, tok_ref.shape[0] // 16, step, 0)


def norm_rows(tokens, gain):
    return pl.pallas_call(
        norm_kernel,
        out_shape=jax.ShapeDtypeStruct(tokens.shape, jnp.bfloat16),
        compiler_params=pltpu.CompilerParams(vmem_limit_bytes=8 * 1024 * 1024),
        cost_estimate=pl.CostEstimate(
            flops=8 * tokens.size, bytes_accessed=4 * tokens.size, transcendentals=0
        ),
    )(tokens, gain[None, :])


def slot(core, k, e):
    odd = (e // CORES) % 2
    return 4 * core + (3, 2 * (1 - odd), 1, 2 * odd)[k]


def block_row(core, k, rows, e):
    return slot(core, k, e) * rows


def row_scale(weights, me, ep):
    count = len(weights)

    def kernel(me_ref, *refs):
        for c in range(CORES):
            for k in range(count):
                row = pl.ds(c * ep + me_ref[0], 1)
                refs[-1][pl.ds(slot(c, k, me_ref[0]), 1)] = refs[k][row]

    shape = (CORES * count, weights[0].shape[1])
    vmem = pl.BlockSpec(memory_space=pltpu.VMEM)
    return pl.pallas_call(
        kernel,
        out_shape=jax.ShapeDtypeStruct(shape, jnp.float32),
        in_specs=[pl.BlockSpec(memory_space=pltpu.SMEM)] + [vmem] * count,
        out_specs=vmem,
        compiler_params=pltpu.CompilerParams(vmem_limit_bytes=4 * 1024 * 1024),
    )(me, *weights)


def column_body(
    tokens,
    norm_gain,
    expert_ids,
    gate_weights,
    expert_gate,
    expert_up,
    expert_down,
    shared_gate,
    shared_up,
    shared_down,
):
    ep, tp = lax.axis_size("ep"), lax.axis_size("tp")
    me = lax.axis_index("ep").astype(jnp.int32)[None]
    tok_rows, features = tokens.shape

    z_up = [(i, (i + CORES) % ep) for i in range(ep)]
    swap, near_z, far_z = ([(i, i ^ step) for i in range(ep)] for step in (1, 2, 4))
    x_swap = [(i, i ^ 1) for i in range(tp)]
    y_swap = [(i, i ^ 2) for i in range(tp)]
    both_swap = [(i, i ^ 3) for i in range(tp)]

    def over_x(a):
        return lax.ppermute(a, "tp", x_swap)

    def over_y(a):
        return lax.ppermute(a, "tp", y_swap)

    def across(a):
        return lax.ppermute(a, "tp", both_swap)

    def up(a):
        return lax.ppermute(a, "ep", z_up)

    def to_near(a):
        return lax.ppermute(a, "ep", near_z)

    def to_far(a):
        return lax.ppermute(a, "ep", far_z)

    def other_core(a):
        return lax.ppermute(a, "ep", swap)

    s = shared_gate.shape[0] // ep
    features = tokens.shape[1]
    every = slice(0, features)
    shared = copy_blocks(
        [(i, lambda e: e * s, s, every, 0, i * s) for i in range(3)],
        (shared_gate, shared_up, shared_down),
        [(3 * s, features)],
        me,
    )[0]
    gate, upw, down = expert_gate[0], expert_up[0], expert_down[0]

    labels = jnp.arange(ep, dtype=jnp.int32)[:, None]
    dense = sum(
        jnp.where(expert_ids[None, :, k] == labels, gate_weights[None, :, k], 0.0)
        for k in range(expert_ids.shape[1])
    )

    gx, gy = over_x(gate), over_y(gate)
    ux, uy = over_x(upw), over_y(upw)
    sx, sy = over_x(shared), over_y(shared)
    gd, ud, sd = over_y(gx), over_x(uy), over_x(sy)

    normed = norm_rows(tokens, norm_gain)
    a1 = to_far(normed)
    own_blocks = [normed, to_near(normed), a1, to_near(a1)]
    other_blocks = [other_core(block) for block in own_blocks]
    pair = jnp.concatenate([dense, other_core(dense)], axis=0)
    w1 = to_far(pair)
    weights = [pair, to_near(pair), w1, to_near(w1)]

    quarter = features // CHUNKS
    down_rows = []
    for n, (lo, hi) in enumerate(((0, 1), (1, 2), (2, 3), (3, 4))):
        piece = down[:, lo * quarter : hi * quarter]
        dx, dy = over_x(piece), over_y(piece)
        dd = across(piece)
        down_rows.append((piece, dx, dy, dd))

    shares = (shared, sx, sy, sd)
    n = gate.shape[0]
    units = 4 * n + 4 * s
    places = (0, n, 2 * n, 3 * n)
    arrays = (gate, gx, gy, gd, upw, ux, uy, ud, *shares)
    jobs = [(i, 0, n, every, i // 4, places[i % 4]) for i in range(8)]
    jobs += [(8 + i, t * s, s, every, t, 4 * n + i * s) for i in range(4) for t in range(2)]
    blocks = (*own_blocks, *other_blocks)
    jobs += [
        (12 + 4 * c + k, 0, tok_rows, every, 2, partial(block_row, c, k, tok_rows))
        for c in range(CORES)
        for k in range(4)
    ]
    shapes = [(units, features)] * 2 + [(8 * tok_rows, features)]
    g_all, u_all, rows = copy_blocks(jobs, (*arrays, *blocks), shapes, me)
    weights = lax.optimization_barrier((*weights, own_blocks[3]))[:-1]
    scale = row_scale(weights, me, ep).reshape(-1, 1)
    routed = (jnp.arange(units) < 4 * n)[None, :]
    value = jax.nn.silu(against(rows, g_all)) * against(rows, u_all)
    hidden = (value * jnp.where(routed, scale, 1.0)).astype(jnp.bfloat16)

    own_rows = 4 * tok_rows

    parts = []
    for pieces in down_rows:
        jobs, count = [], pieces[0].shape[1] // quarter
        for t in range(count):
            cols = slice(t * quarter, (t + 1) * quarter)
            jobs += [(i, 0, n, cols, t, i * n) for i in range(4)]
            at = (len(parts) + t) * quarter
            cols = slice(at, at + quarter)
            jobs += [(4 + i, 2 * s, s, cols, t, 4 * n + i * s) for i in range(4)]
        downs = copy_blocks(jobs, (*pieces, *shares), [(units, quarter)] * count, me)
        for rows_down in downs:
            part = jnp.dot(hidden, rows_down, preferred_element_type=jnp.float32)
            parts.append(with_layout_constraint(part, Layout(major_to_minor=(0, 1))))
    mine, arrived = [], []
    for part in parts:
        swapped = other_core(part[own_rows:].astype(jnp.bfloat16))
        for r in range(1, 4):
            block = part[(r - 1) * tok_rows : r * tok_rows]
            moving = block + swapped[(r - 1) * tok_rows : r * tok_rows].astype(jnp.float32)
            if r > 1:
                moving = moving + came.astype(jnp.float32)
            moving = moving.astype(jnp.bfloat16)
            came = up(moving)
        moving = part[3 * tok_rows : own_rows] + swapped[3 * tok_rows :].astype(jnp.float32)
        mine.append(moving)
        arrived.append(came)
    arrived = lax.optimization_barrier(tuple(arrived))
    outs = [(a + b).astype(jnp.bfloat16) for a, b in zip(mine, arrived)]
    return jnp.concatenate(outs, axis=1)


def solution(mesh):
    ep, tp = mesh.shape["ep"], mesh.shape["tp"]
    columns = tp == 4 and ep == 4 * CORES

    def body(*args):
        return (column_body if columns else exchange_body)(*args)

    in_specs = (
        P(("ep", "tp"), None),
        P(),
        P(("ep", "tp"), None),
        P(("ep", "tp"), None),
        P("ep", "tp", None),
        P("ep", "tp", None),
        P("ep", "tp", None),
        P("tp", None),
        P("tp", None),
        P("tp", None),
    )
    out_specs = P(("ep", "tp"), None)
    return jax.shard_map(
        body, mesh=mesh, in_specs=in_specs, out_specs=out_specs, check_vma=False
    )
```
